32 devices in a mesh: grp: 2 (over y), kv: 4 (over z), tp: 4 (over x, core).
Axes of the slice: x: 2, y: 2, z: 4, core: 2. Of those that a mesh axis runs over, the one named last changes fastest.
Arguments:
- tokens: bfloat16 [64, 4096], P('grp', ('kv', 'tp')), parts along dimension 0, may hold values from -8 to 8
- norm_gain: bfloat16 [4096], P('kv'), may hold values from 0.099609375 to 1.8984375
- w_query: bfloat16 [4096, 1024], P('kv', 'tp'), may hold values from -0.09375 to 0.09375
- w_key: bfloat16 [4096, 1024], P('kv', 'tp'), may hold values from -0.09375 to 0.09375
- w_value: bfloat16 [4096, 2048], P('kv', 'tp'), may hold values from -0.09375 to 0.09375
- w_ogate: bfloat16 [4096, 2048], P('kv', 'tp'), may hold values from -0.09375 to 0.09375
- w_igate: bfloat16 [4096, 16], P('kv', 'tp'), may hold values from -0.09375 to 0.09375
- w_fgate: bfloat16 [4096, 16], P('kv', 'tp'), may hold values from -0.09375 to 0.09375
- igate_bias: float32 [16], P('tp'), may hold values from -1 to 1
- fgate_bias: float32 [16], P('tp'), may hold values from -1 to 4
- state_c: float32 [64, 16, 64, 128], P(('grp', 'kv'), 'tp'), parts along dimension 0, may hold values from -1.5 to 1.5
- state_n: float32 [64, 16, 64], P(('grp', 'kv'), 'tp'), parts along dimension 0, may hold values from -1.5 to 1.5
- state_m: float32 [64, 16], P(('grp', 'kv'), 'tp'), parts along dimension 0, may hold values from -3 to 1
- head_gain: bfloat16 [16, 128], P('tp'), may hold values from 0.099609375 to 1.8984375
- w_out: bfloat16 [2048, 4096], P('tp', 'kv'), may hold values from -0.125 to 0.125
- ffn_gain: bfloat16 [4096], P('kv'), may hold values from 0.099609375 to 1.8984375
- w_gate: bfloat16 [4096, 11008], P('kv', 'tp'), may hold values from -0.09375 to 0.09375
- w_up: bfloat16 [4096, 11008], P('kv', 'tp'), may hold values from -0.09375 to 0.09375
- w_down: bfloat16 [11008, 4096], P('tp', 'kv'), may hold values from -0.0546875 to 0.0546875
Outputs:
- out_tokens: bfloat16 [64, 4096], P('grp', ('kv', 'tp')), parts along dimension 0
- new_c: float32 [64, 16, 64, 128], P(('grp', 'kv'), 'tp'), parts along dimension 0
- new_n: float32 [64, 16, 64], P(('grp', 'kv'), 'tp'), parts along dimension 0
- new_m: float32 [64, 16], P(('grp', 'kv'), 'tp'), parts along dimension 0
The draws below stay inside these ranges and needn't reach their ends.
There are 2 independent parts, one for each index of `grp`. The reference program is written for one: setup_inputs(seed, part) draws one part's arguments, and reference() takes and returns one part's arrays. A program takes and returns all parts, laid end to end along the dimension named above; an argument that names none is the same for every part. Nothing has to cross between parts.
All inputs are finite; a program needn't handle non-finite values.
Results may differ from the reference program's by a relative error of at most 0.017.
Values may be sent and summed in bfloat16 or wider, within the bound.
A program may use at most 64 MiB of HBM per device.

```python
import math
import jax
import jax.numpy as jnp
from jax import lax

D = 4096
HEADS = 16
DK = 64
DV = 128
FF = 11008
SEQS = 32


def draw_tokens(key, part):
    first, second, third = jax.random.split(jax.random.fold_in(key, 11), 3)
    position = jnp.arange(D, dtype=jnp.float32) / D
    column_scale = jnp.exp((position - 0.5) * math.log(3.0)) * jnp.exp(jax.random.uniform(second, (D,), jnp.float32, -0.35, 0.35))
    row_scale = jnp.exp(jax.random.uniform(third, (SEQS, 1), jnp.float32, 0.0, math.log(10.0))) / 3.0
    base = jax.random.normal(first, (SEQS, D), jnp.float32)
    return jnp.clip(base * row_scale * column_scale, -8.0, 8.0).astype(jnp.bfloat16)


def level_of(key, dims, pieces, low, high):
    loudness = 1.0
    for axis_at, parts in pieces:
        steps = jax.random.uniform(jax.random.fold_in(jax.random.fold_in(key, 6), axis_at), (parts,), jnp.float32, low / len(pieces), high / len(pieces))
        loudness = loudness * jnp.repeat(jnp.exp(steps), dims[axis_at] // parts).reshape((-1,) + (1,) * (len(dims) - 1 - axis_at))
    return loudness


def normal_values(key, dims, deviation, most, cuts=(), kind=jnp.bfloat16):
    loudness = level_of(key, dims, cuts, -0.22, 0.18) if cuts else 1.0
    values = jax.random.normal(key, dims, jnp.float32) * deviation * loudness
    return jnp.minimum(jnp.maximum(values, -most), most).astype(kind)


def setup_inputs(seed: int = 0, part: int = 0) -> dict:
    key_list = jax.random.split(jax.random.key(seed), 20)
    own_keys = jax.random.split(jax.random.fold_in(key_list[19], part), 20)
    tokens = draw_tokens(jax.random.fold_in(jax.random.fold_in(key_list[19], part), 71), part)
    norm_gain = jnp.clip(1.0 + 0.18 * jax.random.normal(key_list[1], (D,), jnp.float32), 0.099609375, 1.8984375).astype(jnp.bfloat16)
    w_query = normal_values(key_list[2], (D, HEADS * DK), D ** -0.5, 0.09375, ((0, 4), (1, 4)))
    w_key = normal_values(key_list[3], (D, HEADS * DK), D ** -0.5, 0.09375, ((0, 4), (1, 4)))
    w_value = normal_values(key_list[4], (D, HEADS * DV), D ** -0.5, 0.09375, ((0, 4), (1, 4)))
    w_ogate = normal_values(key_list[5], (D, HEADS * DV), D ** -0.5, 0.09375, ((0, 4), (1, 4)))
    w_igate = normal_values(key_list[6], (D, HEADS), D ** -0.5, 0.09375, ((0, 4), (1, 4)))
    w_fgate = normal_values(key_list[7], (D, HEADS), D ** -0.5, 0.09375, ((0, 4), (1, 4)))
    igate_bias = jnp.clip(jax.random.uniform(key_list[8], (HEADS,), jnp.float32, -1.0, 1.0) * level_of(key_list[8], (HEADS,), ((0, 4),), -0.4, 0.0), -1.0, 1.0)
    fgate_bias = jnp.clip(-1.0 + 5.0 * jax.random.uniform(key_list[9], (HEADS,), jnp.float32) ** level_of(key_list[9], (HEADS,), ((0, 4),), -0.2, 0.2), -1.0, 4.0)
    state_c = normal_values(own_keys[10], (SEQS, HEADS, DK, DV), 0.25, 1.5, ((0, 4), (1, 4)), jnp.float32)
    state_n = normal_values(own_keys[11], (SEQS, HEADS, DK), 0.25, 1.5, ((0, 4), (1, 4)), jnp.float32)
    state_m = jnp.clip(-3.0 + 4.0 * jax.random.uniform(own_keys[12], (SEQS, HEADS), jnp.float32) ** level_of(own_keys[12], (SEQS, HEADS), ((0, 4), (1, 4)), -0.2, 0.2), -3.0, 1.0)
    head_gain = jnp.clip(1.0 + 0.18 * jax.random.normal(key_list[13], (HEADS, DV), jnp.float32), 0.099609375, 1.8984375).astype(jnp.bfloat16)
    w_out = normal_values(key_list[14], (HEADS * DV, D), (HEADS * DV) ** -0.5, 0.125, ((0, 4), (1, 4)))
    ffn_gain = jnp.clip(1.0 + 0.18 * jax.random.normal(key_list[15], (D,), jnp.float32), 0.099609375, 1.8984375).astype(jnp.bfloat16)
    w_gate = normal_values(key_list[16], (D, FF), D ** -0.5, 0.09375, ((0, 4), (1, 4)))
    w_up = normal_values(key_list[17], (D, FF), D ** -0.5, 0.09375, ((0, 4), (1, 4)))
    w_down = normal_values(key_list[18], (FF, D), FF ** -0.5, 0.0546875, ((0, 4), (1, 4)))
    return dict(tokens=tokens, norm_gain=norm_gain, w_query=w_query, w_key=w_key, w_value=w_value, w_ogate=w_ogate, w_igate=w_igate, w_fgate=w_fgate, igate_bias=igate_bias, fgate_bias=fgate_bias, state_c=state_c, state_n=state_n, state_m=state_m, head_gain=head_gain, w_out=w_out, ffn_gain=ffn_gain, w_gate=w_gate, w_up=w_up, w_down=w_down)


norm_eps = 1e-06
igate_cap = 1.5

def cell_update(query, key_vec, value_vec, igate, fgate, state_c, state_n, state_m):
    carried = jax.nn.log_sigmoid(fgate) + state_m
    new_m = jnp.maximum(carried, igate)
    keep_weight = jnp.exp(carried - new_m)
    write_weight = jnp.exp(igate - new_m)
    new_c = keep_weight[..., None, None] * state_c + write_weight[..., None, None] * key_vec[..., :, None] * value_vec[..., None, :]
    new_n = keep_weight[..., None] * state_n + write_weight[..., None] * key_vec
    numerator = jnp.einsum('bhd,bhde->bhe', query, new_c, precision=lax.Precision.HIGHEST)
    denominator = lax.optimization_barrier(jnp.sum(query * new_n, axis=-1))
    head_out = numerator / jnp.maximum(jnp.abs(denominator), jnp.exp(-new_m))[..., None]
    return (new_c, new_n, new_m, head_out)

def reference(tokens, norm_gain, w_query, w_key, w_value, w_ogate, w_igate, w_fgate, igate_bias, fgate_bias, state_c, state_n, state_m, head_gain, w_out, ffn_gain, w_gate, w_up, w_down):
    token_vals = tokens.astype(jnp.float32)
    row_scale = lax.rsqrt(lax.optimization_barrier(jnp.mean(token_vals * token_vals, axis=1, keepdims=True)) + norm_eps)
    normed = (token_vals * norm_gain.astype(jnp.float32)).astype(jnp.bfloat16)

    def project(weight):
        return row_scale * jnp.dot(normed, weight, preferred_element_type=jnp.float32)
    query = project(w_query).reshape(SEQS, HEADS, DK)
    key_vec = project(w_key).reshape(SEQS, HEADS, DK) * DK ** (-0.5)
    value_vec = project(w_value).reshape(SEQS, HEADS, DV)
    ogate = project(w_ogate).reshape(SEQS, HEADS, DV)
    igate = igate_cap * jnp.tanh((project(w_igate) + igate_bias) / igate_cap)
    fgate = project(w_fgate) + fgate_bias
    new_c, new_n, new_m, head_out = cell_update(query, key_vec, value_vec, igate, fgate, state_c, state_n, state_m)
    merged = (head_out * head_gain.astype(jnp.float32) * jax.nn.sigmoid(ogate)).reshape(SEQS, HEADS * DV).astype(jnp.bfloat16)
    attn_out = jnp.dot(merged, w_out, preferred_element_type=jnp.float32)
    middle = (token_vals + attn_out).astype(jnp.bfloat16)
    middle_vals = middle.astype(jnp.float32)
    ffn_scale = lax.rsqrt(lax.optimization_barrier(jnp.mean(middle_vals * middle_vals, axis=1, keepdims=True)) + norm_eps)
    normed_two = (middle_vals * ffn_gain.astype(jnp.float32)).astype(jnp.bfloat16)
    gate_sum = ffn_scale * jnp.dot(normed_two, w_gate, preferred_element_type=jnp.float32)
    up_sum = ffn_scale * jnp.dot(normed_two, w_up, preferred_element_type=jnp.float32)
    hidden = (jax.nn.silu(gate_sum) * up_sum).astype(jnp.bfloat16)
    out_tokens = (middle_vals + jnp.dot(hidden, w_down, preferred_element_type=jnp.float32)).astype(jnp.bfloat16)
    return (out_tokens, new_c, new_n, new_m)
```

```python
import functools

import jax
import jax.numpy as jnp
from jax import lax
from jax.experimental import pallas as pl
from jax.experimental.pallas import tpu as pltpu
from jax.sharding import PartitionSpec as P

F32 = jnp.float32
BF16 = jnp.bfloat16
MESH = pl.DeviceIdType.MESH
NORM_EPS = 1e-06
IGATE_CAP = 1.5
LANES = 128
CHUNK = 768


def cuts(total):
    out = []
    for off in range(0, total, CHUNK):
        width = min(CHUNK, total - off)
        out.append((off, width, -(-width // LANES) * LANES))
    return out


def kernel(
    nkv, ntp, d_model,
    tokens, norm_gain, w_query, w_key, w_value, w_ogate, w_if_i, w_if_f, ib, fb,
    state_c, state_n, state_m, head_gain, w_out, ffn_gain, w_gate, w_up, w_down,
    out_tokens, out_c, out_n, out_m,
    wp, wout, wg, wu, wd, sc, nc,
    tok_all, normed, pj_send, pj_recv, ax_send, ax_recv, num, mg_send, mg_all,
    at_send, at_recv, mid_own, mid_all, sq_send, sq_recv, gu_send, gu_recv, hid_send, hid_all,
    dn_send, dn_recv,
    wsem, osem,
    tok_s, tok_r, pj_s, pj_r, ax_s, ax_r, mg_s, mg_r, at_s, at_r, mid_s, mid_r,
    sq_s, sq_r, gu_s, gu_r, hid_s, hid_r, dn_s, dn_r,
):
    kv = lax.axis_index("kv")
    tp = lax.axis_index("tp")
    kv_peer = [lax.rem(kv + d, nkv) for d in range(1, nkv)]
    tp_peer = [lax.rem(tp + d, ntp) for d in range(1, ntp)]
    kv_src = [lax.rem(kv + nkv - d, nkv) for d in range(1, nkv)]
    tp_src = [lax.rem(tp + ntp - d, ntp) for d in range(1, ntp)]
    seqs = tokens.shape[0]
    rows = seqs // nkv
    tcols = tokens.shape[1]
    heads, dk, dv = state_c.shape[1:]
    qk = w_query.shape[1]
    vv = w_value.shape[1]
    half = qk + vv
    ff = w_gate.shape[0]
    chunks = cuts(ff)

    def fetch(i, src, dst):
        c = pltpu.make_async_copy(src, dst, wsem.at[i])
        c.start()
        return c

    first = [
        fetch(0, w_query, wp.at[:, pl.ds(0, qk)]),
        fetch(1, w_key, wp.at[:, pl.ds(qk, qk)]),
        fetch(2, w_value, wp.at[:, pl.ds(2 * qk, vv)]),
        fetch(3, w_ogate, wp.at[:, pl.ds(2 * qk + vv, vv)]),
    ]

    barrier = pltpu.get_barrier_semaphore()
    for p in kv_peer:
        pl.semaphore_signal(barrier, inc=1, device_id={"kv": p}, device_id_type=MESH)
    for p in tp_peer:
        pl.semaphore_signal(barrier, inc=1, device_id={"tp": p}, device_id_type=MESH)
    pl.semaphore_wait(barrier, nkv - 1 + ntp - 1)

    def send(src, dst, ssem, rsem, dev):
        c = pltpu.make_async_remote_copy(
            src_ref=src, dst_ref=dst, send_sem=ssem, recv_sem=rsem,
            device_id=dev, device_id_type=MESH,
        )
        c.start()
        return c

    pending = []

    copies = [
        send(tokens, tok_all.at[tp], tok_s.at[d], tok_r.at[d], {"tp": p})
        for d, p in enumerate(tp_peer)
    ]
    pending += copies
    tok_all[tp] = tokens[...]
    for c in copies:
        c.wait_recv()
    sq = jnp.zeros((seqs, 1), F32)
    for j in range(ntp):
        t = tok_all[j].astype(F32)
        sl = slice(j * tcols, (j + 1) * tcols)
        normed[:, sl] = (t * norm_gain[:, sl].astype(F32)).astype(BF16)
        sq = sq + jnp.sum(t * t, axis=1, keepdims=True)
    x = normed[...]
    nt = (((1,), (1,)), ((), ()))
    gi = lax.dot_general(x, w_if_i[...], nt, preferred_element_type=F32)
    gf = lax.dot_general(x, w_if_f[...], nt, preferred_element_type=F32)
    lane = lax.broadcasted_iota(jnp.int32, (seqs, LANES), 1)
    aux = jnp.where(lane == 2 * heads, sq, 0.0)
    for h in range(heads):
        aux = jnp.where(lane == h, gi[:, h : h + 1], aux)
        aux = jnp.where(lane == heads + h, gf[:, h : h + 1], aux)
    for k in range(nkv):
        ax_send[k] = aux[k * rows : (k + 1) * rows]
    copies = [
        send(ax_send.at[p], ax_recv.at[kv], ax_s.at[d], ax_r.at[d], {"kv": p})
        for d, p in enumerate(kv_peer)
    ]
    pending += copies
    ax_copies = copies

    for c in first:
        c.wait()
    late = [
        fetch(4, state_c, sc),
        fetch(5, w_out, wout),
        fetch(6, w_gate, wg),
        fetch(7, w_up, wu),
        fetch(8, w_down, wd),
    ]
    lo = jnp.dot(x, wp[:, :half], preferred_element_type=F32)
    hi = jnp.dot(x, wp[:, half:], preferred_element_type=F32)
    for k in range(nkv):
        r = slice(k * rows, (k + 1) * rows)
        pj_send[k] = jnp.concatenate([lo[r], hi[r]], axis=0).astype(BF16)
    copies = [
        send(pj_send.at[p], pj_recv.at[kv], pj_s.at[d], pj_r.at[d], {"kv": p})
        for d, p in enumerate(kv_peer)
    ]
    pending += copies

    a = ax_send[kv]
    for d, c in enumerate(ax_copies):
        c.wait_recv()
        a = a + ax_recv[kv_src[d]]
    row_scale = lax.rsqrt(a[:, 2 * heads : 2 * heads + 1] / d_model + NORM_EPS)
    igate = IGATE_CAP * jnp.tanh((row_scale * a[:, :heads] + ib[...]) / IGATE_CAP)
    fgate = row_scale * a[:, heads : 2 * heads] + fb[...]
    log_sig = jnp.minimum(fgate, 0.0) - jnp.log1p(jnp.exp(-jnp.abs(fgate)))
    carried = log_sig + state_m[...].T
    new_m = jnp.maximum(carried, igate)
    keep = jnp.exp(carried - new_m)
    write = jnp.exp(igate - new_m)
    floor = jnp.exp(-new_m)
    out_m[...] = new_m.T
    late[0].wait()

    s = pj_send[kv].astype(F32)
    for d, c in enumerate(copies):
        c.wait_recv()
        s = s + pj_recv[kv_src[d]].astype(F32)

    def piece(off, width):
        top = off // half
        return s[top * rows : (top + 1) * rows, off - top * half : off - top * half + width]

    q = row_scale * piece(0, qk)
    klane = lax.broadcasted_iota(jnp.int32, (rows, qk), 1) // dk
    spread = jnp.zeros((rows, qk), F32)
    for h in range(heads):
        spread = jnp.where(klane == h, write[:, h : h + 1], spread)
    kw = spread * (row_scale * piece(qk, qk) * dk ** (-0.5))
    q_t = q.T
    k_t = kw.T
    for h in range(heads):
        hk = slice(h * dk, (h + 1) * dk)
        hv = slice(h * dv, (h + 1) * dv)
        keep_h = jnp.broadcast_to(keep[:, h : h + 1], (rows, dv))
        val = row_scale * piece(2 * qk + h * dv, dv)
        for b in range(rows):
            c_new = keep_h[b : b + 1] * sc[b, h] + k_t[hk, b : b + 1] * val[b : b + 1]
            nc[b, h] = c_new
            num[b : b + 1, hv] = jnp.sum(q_t[hk, b : b + 1] * c_new, axis=0, keepdims=True)
        n_new = keep[:, h : h + 1] * state_n[:, h, :] + kw[:, hk]
        out_n[:, h, :] = n_new
        den = jnp.sum(q[:, hk] * n_new, axis=1, keepdims=True)
        head_out = num[:, hv] / jnp.maximum(jnp.abs(den), floor[:, h : h + 1])
        og = row_scale * piece(2 * qk + vv + h * dv, dv)
        gated = head_out * head_gain[h : h + 1].astype(F32) * jax.nn.sigmoid(og)
        mg_send[:, hv] = gated.astype(BF16)
    copies = [
        send(mg_send, mg_all.at[kv], mg_s.at[d], mg_r.at[d], {"kv": p})
        for d, p in enumerate(kv_peer)
    ]
    pending += copies
    c_out = pltpu.make_async_copy(nc, out_c, osem)
    c_out.start()
    mg_all[kv] = mg_send[...]
    late[1].wait()
    for c in copies:
        c.wait_recv()
    merged = jnp.concatenate([mg_all[k].astype(F32) for k in range(nkv)], axis=0).astype(BF16)

    attn = jnp.dot(merged, wout[...], preferred_element_type=F32)
    for j in range(ntp):
        at_send[j] = attn[:, j * tcols : (j + 1) * tcols].astype(BF16)
    copies = [
        send(at_send.at[p], at_recv.at[tp], at_s.at[d], at_r.at[d], {"tp": p})
        for d, p in enumerate(tp_peer)
    ]
    pending += copies
    tot = at_send[tp].astype(F32)
    for d, c in enumerate(copies):
        c.wait_recv()
        tot = tot + at_recv[tp_src[d]].astype(F32)
    mid_own[...] = (tokens[...].astype(F32) + tot).astype(BF16)
    copies = [
        send(mid_own, mid_all.at[tp], mid_s.at[d], mid_r.at[d], {"tp": p})
        for d, p in enumerate(tp_peer)
    ]
    pending += copies
    mid_all[tp] = mid_own[...]
    if chunks[-1][1] != chunks[-1][2]:
        pad = chunks[-1][2] - chunks[-1][1]
        gu_send[:, :, ff:] = jnp.zeros((nkv, 2 * rows, pad), BF16)
        hid_send[:, ff:] = jnp.zeros((rows, pad), BF16)
    late[2].wait()
    late[3].wait()
    for c in copies:
        c.wait_recv()
    sq = jnp.zeros((seqs, 1), F32)
    for j in range(ntp):
        t = mid_all[j].astype(F32)
        sl = slice(j * tcols, (j + 1) * tcols)
        normed[:, sl] = (t * ffn_gain[:, sl].astype(F32)).astype(BF16)
        sq = sq + jnp.sum(t * t, axis=1, keepdims=True)
    sq = jnp.broadcast_to(sq, (seqs, LANES))
    for k in range(nkv):
        sq_send[k] = sq[k * rows : (k + 1) * rows]
    sq_copies = [
        send(sq_send.at[p], sq_recv.at[kv], sq_s.at[d], sq_r.at[d], {"kv": p})
        for d, p in enumerate(kv_peer)
    ]
    pending += sq_copies

    x = normed[...]
    gu_copies = []
    for i, (off, width, wide) in enumerate(chunks):
        g = lax.dot_general(x, wg[off : off + width], nt, preferred_element_type=F32)
        u = lax.dot_general(x, wu[off : off + width], nt, preferred_element_type=F32)
        for k in range(nkv):
            r = slice(k * rows, (k + 1) * rows)
            gu_send[k, :, off : off + width] = jnp.concatenate([g[r], u[r]], axis=0).astype(BF16)
        window = pl.ds(off, wide)
        copies = [
            send(gu_send.at[p, :, window], gu_recv.at[kv, :, window],
                 gu_s.at[i, d], gu_r.at[i, d], {"kv": p})
            for d, p in enumerate(kv_peer)
        ]
        gu_copies.append(copies)
        pending += copies

    a = sq_send[kv]
    for d, c in enumerate(sq_copies):
        c.wait_recv()
        a = a + sq_recv[kv_src[d]]
    ffn_scale = lax.rsqrt(a[:, :1] / d_model + NORM_EPS)
    hid_copies = []
    for i, (off, width, wide) in enumerate(chunks):
        t = gu_send[kv, :, off : off + wide].astype(F32)
        for d, c in enumerate(gu_copies[i]):
            c.wait_recv()
            t = t + gu_recv[kv_src[d], :, off : off + wide].astype(F32)
        g = ffn_scale * t[:rows]
        hid = g / (1.0 + jnp.exp(-g)) * (ffn_scale * t[rows:])
        hid_send[:, off : off + wide] = hid.astype(BF16)
        window = pl.ds(off, wide)
        copies = [
            send(hid_send.at[:, window], hid_all.at[kv, :, window],
                 hid_s.at[i, d], hid_r.at[i, d], {"kv": p})
            for d, p in enumerate(kv_peer)
        ]
        hid_copies.append(copies)
        pending += copies
    hid_all[kv] = hid_send[...]
    late[4].wait()
    down = None
    for i, (off, width, wide) in enumerate(chunks):
        for c in hid_copies[i]:
            c.wait_recv()
        h = jnp.concatenate(
            [hid_all[k, :, off : off + width].astype(F32) for k in range(nkv)], axis=0
        ).astype(BF16)
        part = jnp.dot(h, wd[off : off + width, :], preferred_element_type=F32)
        down = part if down is None else down + part
    for j in range(ntp):
        dn_send[j] = down[:, j * tcols : (j + 1) * tcols].astype(BF16)
    copies = [
        send(dn_send.at[p], dn_recv.at[tp], dn_s.at[d], dn_r.at[d], {"tp": p})
        for d, p in enumerate(tp_peer)
    ]
    pending += copies
    tot = dn_send[tp].astype(F32)
    for d, c in enumerate(copies):
        c.wait_recv()
        tot = tot + dn_recv[tp_src[d]].astype(F32)
    out_tokens[...] = (mid_own[...].astype(F32) + tot).astype(BF16)
    for c in pending:
        c.wait_send()
    c_out.wait()


def layer(
    nkv, ntp, d_model,
    tokens, norm_gain, w_query, w_key, w_value, w_ogate, w_igate, w_fgate,
    igate_bias, fgate_bias, state_c, state_n, state_m, head_gain,
    w_out, ffn_gain, w_gate, w_up, w_down,
):
    seqs, tcols = tokens.shape
    rows = seqs // nkv
    depth, qk = w_query.shape
    vv = w_value.shape[1]
    half = qk + vv
    ff = w_gate.shape[1]
    nch = len(cuts(ff))
    wide = -(-ff // LANES) * LANES
    hbm = pl.BlockSpec(memory_space=pl.ANY)
    vmem = pl.BlockSpec(memory_space=pltpu.VMEM)
    dma = lambda *n: pltpu.SemaphoreType.DMA(n)
    k, t = nkv - 1, ntp - 1
    scratch = [
        pltpu.VMEM((depth, 2 * half), BF16),
        pltpu.VMEM(w_out.shape, BF16),
        pltpu.VMEM(w_gate.shape[::-1], BF16),
        pltpu.VMEM(w_up.shape[::-1], BF16),
        pltpu.VMEM(w_down.shape, BF16),
        pltpu.VMEM(state_c.shape, F32),
        pltpu.VMEM(state_c.shape, F32),
        pltpu.VMEM((ntp, seqs, tcols), BF16),
        pltpu.VMEM((seqs, depth), BF16),
        pltpu.VMEM((nkv, 2 * rows, half), BF16),
        pltpu.VMEM((nkv, 2 * rows, half), BF16),
        pltpu.VMEM((nkv, rows, LANES), F32),
        pltpu.VMEM((nkv, rows, LANES), F32),
        pltpu.VMEM((rows, vv), F32),
        pltpu.VMEM((rows, vv), BF16),
        pltpu.VMEM((nkv, rows, vv), BF16),
        pltpu.VMEM((ntp, seqs, tcols), BF16),
        pltpu.VMEM((ntp, seqs, tcols), BF16),
        pltpu.VMEM((seqs, tcols), BF16),
        pltpu.VMEM((ntp, seqs, tcols), BF16),
        pltpu.VMEM((nkv, rows, LANES), F32),
        pltpu.VMEM((nkv, rows, LANES), F32),
        pltpu.VMEM((nkv, 2 * rows, wide), BF16),
        pltpu.VMEM((nkv, 2 * rows, wide), BF16),
        pltpu.VMEM((rows, wide), BF16),
        pltpu.VMEM((nkv, rows, wide), BF16),
        pltpu.VMEM((ntp, seqs, tcols), BF16),
        pltpu.VMEM((ntp, seqs, tcols), BF16),
        dma(9),
        pltpu.SemaphoreType.DMA,
        dma(t), dma(t), dma(k), dma(k), dma(k), dma(k), dma(k), dma(k), dma(t), dma(t), dma(t), dma(t),
        dma(k), dma(k), dma(nch, k), dma(nch, k), dma(nch, k), dma(nch, k), dma(t), dma(t),
    ]
    in_specs = [
        vmem, vmem, hbm, hbm, hbm, hbm, vmem, vmem, vmem, vmem,
        hbm, vmem, vmem, vmem, hbm, vmem, hbm, hbm, hbm,
    ]
    out = pl.pallas_call(
        functools.partial(kernel, nkv, ntp, d_model),
        out_shape=(
            jax.ShapeDtypeStruct(tokens.shape, BF16),
            jax.ShapeDtypeStruct(state_c.shape, F32),
            jax.ShapeDtypeStruct(state_n.shape, F32),
            jax.ShapeDtypeStruct(state_m.shape[::-1], F32),
        ),
        in_specs=in_specs,
        out_specs=(vmem, hbm, vmem, vmem),
        scratch_shapes=scratch,
        compiler_params=pltpu.CompilerParams(
            collective_id=0, has_side_effects=True, vmem_limit_bytes=60 * 1024 * 1024
        ),
    )(
        tokens, norm_gain[None], w_query, w_key, w_value, w_ogate, w_igate.T, w_fgate.T,
        igate_bias[None], fgate_bias[None], state_c, state_n, state_m.T, head_gain,
        w_out, ffn_gain[None], w_gate.T, w_up.T, w_down,
    )
    return (*out[:3], out[3].T)


def cell_update(query, key_vec, value_vec, igate, fgate, state_c, state_n, state_m):
    carried = jax.nn.log_sigmoid(fgate) + state_m
    new_m = jnp.maximum(carried, igate)
    keep_weight = jnp.exp(carried - new_m)
    write_weight = jnp.exp(igate - new_m)
    new_c = (
        keep_weight[..., None, None] * state_c
        + write_weight[..., None, None] * key_vec[..., :, None] * value_vec[..., None, :]
    )
    new_n = keep_weight[..., None] * state_n + write_weight[..., None] * key_vec
    numerator = jnp.einsum("bhd,bhde->bhe", query, new_c, precision=lax.Precision.HIGHEST)
    denominator = jnp.sum(query * new_n, axis=-1)
    head_out = numerator / jnp.maximum(jnp.abs(denominator), jnp.exp(-new_m))[..., None]
    return (new_c, new_n, new_m, head_out)


def plain_layer(
    tokens,
    norm_gain,
    w_query,
    w_key,
    w_value,
    w_ogate,
    w_igate,
    w_fgate,
    igate_bias,
    fgate_bias,
    state_c,
    state_n,
    state_m,
    head_gain,
    w_out,
    ffn_gain,
    w_gate,
    w_up,
    w_down,
):
    seq_rows = state_c.shape[0]
    heads_here, DK, DV = state_c.shape[1:]
    D = w_query.shape[0] * lax.axis_size("kv")
    token_cols = lax.all_gather(tokens, "tp", axis=1, tiled=True)
    token_vals = token_cols.astype(jnp.float32)
    normed = (token_vals * norm_gain.astype(jnp.float32)).astype(jnp.bfloat16)
    squares = jnp.sum(token_vals * token_vals, axis=1)
    part_query = jnp.dot(normed, w_query, preferred_element_type=jnp.float32)
    part_key = jnp.dot(normed, w_key, preferred_element_type=jnp.float32)
    part_value = jnp.dot(normed, w_value, preferred_element_type=jnp.float32)
    part_ogate = jnp.dot(normed, w_ogate, preferred_element_type=jnp.float32)
    part_igate = jnp.dot(normed, w_igate, preferred_element_type=jnp.float32)
    part_fgate = jnp.dot(normed, w_fgate, preferred_element_type=jnp.float32)
    all_squares = lax.psum(squares, "kv")
    sum_squares = lax.dynamic_slice_in_dim(
        all_squares, lax.axis_index("kv") * seq_rows, seq_rows, 0
    )
    sum_query, sum_key, sum_value, sum_ogate, sum_igate, sum_fgate = (
        lax.psum_scatter(part_query, "kv", scatter_dimension=0, tiled=True),
        lax.psum_scatter(part_key, "kv", scatter_dimension=0, tiled=True),
        lax.psum_scatter(part_value, "kv", scatter_dimension=0, tiled=True),
        lax.psum_scatter(part_ogate, "kv", scatter_dimension=0, tiled=True),
        lax.psum_scatter(part_igate, "kv", scatter_dimension=0, tiled=True),
        lax.psum_scatter(part_fgate, "kv", scatter_dimension=0, tiled=True),
    )
    row_scale = lax.rsqrt(sum_squares / D + NORM_EPS)[:, None]
    query = (row_scale * sum_query).reshape(seq_rows, heads_here, DK)
    key_vec = (row_scale * sum_key).reshape(seq_rows, heads_here, DK) * DK ** (-0.5)
    value_vec = (row_scale * sum_value).reshape(seq_rows, heads_here, DV)
    ogate = (row_scale * sum_ogate).reshape(seq_rows, heads_here, DV)
    igate = IGATE_CAP * jnp.tanh((row_scale * sum_igate + igate_bias) / IGATE_CAP)
    fgate = row_scale * sum_fgate + fgate_bias
    new_c, new_n, new_m, head_out = cell_update(
        query, key_vec, value_vec, igate, fgate, state_c, state_n, state_m
    )
    merged = (
        (head_out * head_gain.astype(jnp.float32) * jax.nn.sigmoid(ogate))
        .reshape(seq_rows, heads_here * DV)
        .astype(jnp.bfloat16)
    )
    attn_part = jnp.dot(
        lax.all_gather(merged, "kv", axis=0, tiled=True), w_out, preferred_element_type=jnp.float32
    )
    attn_out = lax.psum_scatter(
        attn_part.astype(jnp.bfloat16), "tp", scatter_dimension=1, tiled=True
    ).astype(jnp.float32)
    middle = (tokens.astype(jnp.float32) + attn_out).astype(jnp.bfloat16)
    middle_cols = lax.all_gather(middle, "tp", axis=1, tiled=True)
    middle_vals = middle_cols.astype(jnp.float32)
    normed_two = (middle_vals * ffn_gain.astype(jnp.float32)).astype(jnp.bfloat16)
    squares_two = jnp.sum(middle_vals * middle_vals, axis=1)
    gate_part = jnp.dot(normed_two, w_gate, preferred_element_type=jnp.float32)
    up_part = jnp.dot(normed_two, w_up, preferred_element_type=jnp.float32)
    gate_sum, up_sum, total_two = (
        lax.psum(gate_part.astype(jnp.bfloat16), "kv").astype(jnp.float32),
        lax.psum(up_part.astype(jnp.bfloat16), "kv").astype(jnp.float32),
        lax.psum(squares_two.astype(jnp.bfloat16), "kv").astype(jnp.float32),
    )
    ffn_scale = lax.rsqrt(total_two / D + NORM_EPS)[:, None]
    hidden = (jax.nn.silu(ffn_scale * gate_sum) * (ffn_scale * up_sum)).astype(jnp.bfloat16)
    down_part = jnp.dot(hidden, w_down, preferred_element_type=jnp.float32)
    down_out = lax.psum_scatter(
        down_part.astype(jnp.bfloat16), "tp", scatter_dimension=1, tiled=True
    ).astype(jnp.float32)
    out_tokens = (middle.astype(jnp.float32) + down_out).astype(jnp.bfloat16)
    return (out_tokens, new_c, new_n, new_m)


def solution(mesh):
    nkv, ntp = mesh.shape["kv"], mesh.shape["tp"]
    placed = (
        P("grp", ("kv", "tp")),
        P("kv"),
        P("kv", "tp"),
        P("kv", "tp"),
        P("kv", "tp"),
        P("kv", "tp"),
        P("kv", "tp"),
        P("kv", "tp"),
        P("tp"),
        P("tp"),
        P(("grp", "kv"), "tp", None, None),
        P(("grp", "kv"), "tp", None),
        P(("grp", "kv"), "tp"),
        P("tp", None),
        P("tp", "kv"),
        P("kv"),
        P("kv", "tp"),
        P("kv", "tp"),
        P("tp", "kv"),
    )

    def body(*args):
        d_model = args[2].shape[0] * nkv
        seqs, tcols = args[0].shape
        qk, vv = args[2].shape[1], args[4].shape[1]
        whole_tiles = tcols % LANES == 0 and qk % LANES == 0 and vv % LANES == 0
        if not whole_tiles or (seqs // nkv) % 8:
            return plain_layer(*args)
        return layer(nkv, ntp, d_model, *args)

    return jax.shard_map(
        body,
        mesh=mesh,
        in_specs=placed,
        out_specs=(
            P("grp", ("kv", "tp")),
            P(("grp", "kv"), "tp", None, None),
            P(("grp", "kv"), "tp", None),
            P(("grp", "kv"), "tp"),
        ),
        check_vma=False,
    )
```

```python
import functools

import jax
import jax.numpy as jnp
from jax import lax
from jax.experimental import pallas as pl
from jax.experimental.pallas import tpu as pltpu
from jax.sharding import PartitionSpec as P

F32 = jnp.float32
BF16 = jnp.bfloat16
MESH = pl.DeviceIdType.MESH
NORM_EPS = 1e-06
IGATE_CAP = 1.5
LANES = 128
CHUNK = 768
PARTS = 4


def cuts(total):
    out = []
    for off in range(0, total, CHUNK):
        width = min(CHUNK, total - off)
        out.append((off, width, -(-width // LANES) * LANES))
    return out


def kernel(
    nkv, ntp, d_model,
    tokens_in, norm_gain_in, w_query, w_key, w_value, w_ogate, w_if_i_in, w_if_f_in, ib_in, fb_in,
    state_c, state_n_in, state_m_in, head_gain_in, w_out, ffn_gain_in, w_gate, w_up, w_down,
    out_tokens, out_c, out_n, out_m,
    tokens, norm_gain, w_if_i, w_if_f, ib, fb, state_n, state_m, head_gain, ffn_gain,
    wp, wout, wg, wu, wd, sc, nc,
    tok_all, normed, pj_send, pj_recv, ax_send, ax_recv, num, mg_send, mg_all,
    at_send, at_recv, mid_own, mid_all, sq_send, sq_recv, gu_send, gu_recv, hid_send, hid_all,
    dn_send, dn_recv,
    wsem, osem, small_sem,
    tok_s, tok_r, pj_s, pj_r, ax_s, ax_r, mg_s, mg_r, at_s, at_r, mid_s, mid_r,
    sq_s, sq_r, gu_s, gu_r, hid_s, hid_r, dn_s, dn_r,
):
    kv = lax.axis_index("kv")
    tp = lax.axis_index("tp")
    kv_peer = [lax.rem(kv + d, nkv) for d in range(1, nkv)]
    tp_peer = [lax.rem(tp + d, ntp) for d in range(1, ntp)]
    kv_src = [lax.rem(kv + nkv - d, nkv) for d in range(1, nkv)]
    tp_src = [lax.rem(tp + ntp - d, ntp) for d in range(1, ntp)]
    seqs = tokens.shape[0]
    rows = seqs // nkv
    tcols = tokens.shape[1]
    heads, dk, dv = state_c.shape[1:]
    qk = w_query.shape[1]
    vv = w_value.shape[1]
    half = qk + vv
    ff = w_gate.shape[0]
    chunks = cuts(ff)

    barrier = pltpu.get_barrier_semaphore()
    for p in kv_peer:
        pl.semaphore_signal(barrier, inc=1, device_id={"kv": p}, device_id_type=MESH)
    for p in tp_peer:
        pl.semaphore_signal(barrier, inc=1, device_id={"tp": p}, device_id_type=MESH)

    def fetch(i, src, dst):
        c = pltpu.make_async_copy(src, dst, wsem.at[i])
        c.start()
        return c

    small = []
    for i, (src, dst) in enumerate([
        (tokens_in, tokens), (norm_gain_in, norm_gain), (w_if_i_in, w_if_i), (w_if_f_in, w_if_f),
        (ib_in, ib), (fb_in, fb), (state_n_in, state_n), (state_m_in, state_m),
        (head_gain_in, head_gain), (ffn_gain_in, ffn_gain),
    ]):
        c = pltpu.make_async_copy(src, dst, small_sem.at[i])
        c.start()
        small.append(c)
    first = [
        fetch(0, w_query, wp.at[:, pl.ds(0, qk)]),
        fetch(1, w_key, wp.at[:, pl.ds(qk, qk)]),
        fetch(2, w_value, wp.at[:, pl.ds(2 * qk, vv)]),
        fetch(3, w_ogate, wp.at[:, pl.ds(2 * qk + vv, vv)]),
    ]

    small[0].wait()
    pl.semaphore_wait(barrier, nkv - 1 + ntp - 1)

    def send(src, dst, ssem, rsem, dev):
        c = pltpu.make_async_remote_copy(
            src_ref=src, dst_ref=dst, send_sem=ssem, recv_sem=rsem,
            device_id=dev, device_id_type=MESH,
        )
        c.start()
        return c

    def scaled(t, j, gain):
        for c in range(tcols // LANES):
            g = j * (tcols // LANES) + c
            part = t[:, c * LANES : (c + 1) * LANES] * gain[g : g + 1].astype(F32)
            normed[:, g * LANES : (g + 1) * LANES] = part.astype(BF16)

    pending = []

    copies = [
        send(tokens, tok_all.at[tp], tok_s.at[d], tok_r.at[d], {"tp": p})
        for d, p in enumerate(tp_peer)
    ]
    pending += copies
    tok_all[tp] = tokens[...]
    for c in small[1:]:
        c.wait()
    for c in copies:
        c.wait_recv()
    sq = jnp.zeros((seqs, 1), F32)
    for j in range(ntp):
        t = tok_all[j].astype(F32)
        scaled(t, j, norm_gain)
        sq = sq + jnp.sum(t * t, axis=1, keepdims=True)
    x = normed[...]
    nt = (((1,), (1,)), ((), ()))
    gi = lax.dot_general(x, w_if_i[...], nt, preferred_element_type=F32)
    gf = lax.dot_general(x, w_if_f[...], nt, preferred_element_type=F32)
    lane = lax.broadcasted_iota(jnp.int32, (seqs, LANES), 1)
    aux = jnp.where(lane == 2 * heads, sq, 0.0)
    for h in range(heads):
        aux = jnp.where(lane == h, gi[:, h : h + 1], aux)
        aux = jnp.where(lane == heads + h, gf[:, h : h + 1], aux)
    for k in range(nkv):
        ax_send[k] = aux[k * rows : (k + 1) * rows]
    copies = [
        send(ax_send.at[p], ax_recv.at[kv], ax_s.at[d], ax_r.at[d], {"kv": p})
        for d, p in enumerate(kv_peer)
    ]
    pending += copies
    ax_copies = copies

    for c in first:
        c.wait()
    late = [
        fetch(4, state_c, sc),
        fetch(5, w_out, wout),
        fetch(6, w_gate, wg),
        fetch(7, w_up, wu),
        fetch(8, w_down, wd),
    ]
    lo = jnp.dot(x, wp[:, :half], preferred_element_type=F32)
    hi = jnp.dot(x, wp[:, half:], preferred_element_type=F32)
    for k in range(nkv):
        r = slice(k * rows, (k + 1) * rows)
        pj_send[k] = jnp.concatenate([lo[r], hi[r]], axis=0).astype(BF16)
    copies = [
        send(pj_send.at[p], pj_recv.at[kv], pj_s.at[d], pj_r.at[d], {"kv": p})
        for d, p in enumerate(kv_peer)
    ]
    pending += copies

    a = ax_send[kv]
    for d, c in enumerate(ax_copies):
        c.wait_recv()
        a = a + ax_recv[kv_src[d]]
    row_scale = lax.rsqrt(a[:, 2 * heads : 2 * heads + 1] / d_model + NORM_EPS)
    igate = IGATE_CAP * jnp.tanh((row_scale * a[:, :heads] + ib[...]) / IGATE_CAP)
    fgate = row_scale * a[:, heads : 2 * heads] + fb[...]
    log_sig = jnp.minimum(fgate, 0.0) - jnp.log1p(jnp.exp(-jnp.abs(fgate)))
    carried = log_sig + state_m[...].T
    new_m = jnp.maximum(carried, igate)
    keep = jnp.exp(carried - new_m)
    write = jnp.exp(igate - new_m)
    floor = jnp.exp(-new_m)
    out_m[...] = new_m.T
    late[0].wait()

    s = pj_send[kv].astype(F32)
    for d, c in enumerate(copies):
        c.wait_recv()
        s = s + pj_recv[kv_src[d]].astype(F32)

    def piece(off, width):
        top = off // half
        return s[top * rows : (top + 1) * rows, off - top * half : off - top * half + width]

    q = row_scale * piece(0, qk)
    klane = lax.broadcasted_iota(jnp.int32, (rows, qk), 1) // dk
    spread = jnp.zeros((rows, qk), F32)
    for h in range(heads):
        spread = jnp.where(klane == h, write[:, h : h + 1], spread)
    kw = spread * (row_scale * piece(qk, qk) * dk ** (-0.5))
    q_t = q.T
    k_t = kw.T
    for h in range(heads):
        hk = slice(h * dk, (h + 1) * dk)
        hv = slice(h * dv, (h + 1) * dv)
        keep_h = jnp.broadcast_to(keep[:, h : h + 1], (rows, dv))
        val = row_scale * piece(2 * qk + h * dv, dv)
        for b in range(rows):
            c_new = keep_h[b : b + 1] * sc[b, h] + k_t[hk, b : b + 1] * val[b : b + 1]
            nc[b, h] = c_new
            num[b : b + 1, hv] = jnp.sum(q_t[hk, b : b + 1] * c_new, axis=0, keepdims=True)
        n_new = keep[:, h : h + 1] * state_n[:, h, :] + kw[:, hk]
        out_n[:, h, :] = n_new
        den = jnp.sum(q[:, hk] * n_new, axis=1, keepdims=True)
        head_out = num[:, hv] / jnp.maximum(jnp.abs(den), floor[:, h : h + 1])
        og = row_scale * piece(2 * qk + vv + h * dv, dv)
        gated = head_out * head_gain[h : h + 1].astype(F32) * jax.nn.sigmoid(og)
        mg_send[:, hv] = gated.astype(BF16)
    copies = [
        send(mg_send, mg_all.at[kv], mg_s.at[d], mg_r.at[d], {"kv": p})
        for d, p in enumerate(kv_peer)
    ]
    pending += copies
    c_out = pltpu.make_async_copy(nc, out_c, osem)
    c_out.start()
    mg_all[kv] = mg_send[...]
    late[1].wait()
    for c in copies:
        c.wait_recv()
    merged = jnp.concatenate([mg_all[k].astype(F32) for k in range(nkv)], axis=0).astype(BF16)

    attn = jnp.dot(merged, wout[...], preferred_element_type=F32)
    for j in range(ntp):
        at_send[j] = attn[:, j * tcols : (j + 1) * tcols].astype(BF16)
    copies = [
        send(at_send.at[p], at_recv.at[tp], at_s.at[d], at_r.at[d], {"tp": p})
        for d, p in enumerate(tp_peer)
    ]
    pending += copies
    tot = at_send[tp].astype(F32)
    for d, c in enumerate(copies):
        c.wait_recv()
        tot = tot + at_recv[tp_src[d]].astype(F32)
    mid_own[...] = (tokens[...].astype(F32) + tot).astype(BF16)
    copies = [
        send(mid_own, mid_all.at[tp], mid_s.at[d], mid_r.at[d], {"tp": p})
        for d, p in enumerate(tp_peer)
    ]
    pending += copies
    mid_all[tp] = mid_own[...]
    if chunks[-1][1] != chunks[-1][2]:
        pad = chunks[-1][2] - chunks[-1][1]
        gu_send[:, :, ff:] = jnp.zeros((nkv, 2 * rows, pad), BF16)
        hid_send[:, ff:] = jnp.zeros((rows, pad), BF16)
    late[2].wait()
    late[3].wait()
    for c in copies:
        c.wait_recv()
    sq = jnp.zeros((seqs, 1), F32)
    for j in range(ntp):
        t = mid_all[j].astype(F32)
        scaled(t, j, ffn_gain)
        sq = sq + jnp.sum(t * t, axis=1, keepdims=True)
    sq = jnp.broadcast_to(sq, (seqs, LANES))
    for k in range(nkv):
        sq_send[k] = sq[k * rows : (k + 1) * rows]
    sq_copies = [
        send(sq_send.at[p], sq_recv.at[kv], sq_s.at[d], sq_r.at[d], {"kv": p})
        for d, p in enumerate(kv_peer)
    ]
    pending += sq_copies

    x = normed[...]
    gu_copies = []
    for i, (off, width, wide) in enumerate(chunks):
        g = lax.dot_general(x, wg[off : off + width], nt, preferred_element_type=F32)
        u = lax.dot_general(x, wu[off : off + width], nt, preferred_element_type=F32)
        for k in range(nkv):
            r = slice(k * rows, (k + 1) * rows)
            gu_send[k, :, off : off + width] = jnp.concatenate([g[r], u[r]], axis=0).astype(BF16)
        window = pl.ds(off, wide)
        copies = [
            send(gu_send.at[p, :, window], gu_recv.at[kv, :, window],
                 gu_s.at[i, d], gu_r.at[i, d], {"kv": p})
            for d, p in enumerate(kv_peer)
        ]
        gu_copies.append(copies)
        pending += copies

    a = sq_send[kv]
    for d, c in enumerate(sq_copies):
        c.wait_recv()
        a = a + sq_recv[kv_src[d]]
    ffn_scale = lax.rsqrt(a[:, :1] / d_model + NORM_EPS)
    hid_copies = []
    for i, (off, width, wide) in enumerate(chunks):
        t = gu_send[kv, :, off : off + wide].astype(F32)
        for d, c in enumerate(gu_copies[i]):
            c.wait_recv()
            t = t + gu_recv[kv_src[d], :, off : off + wide].astype(F32)
        g = ffn_scale * t[:rows]
        hid = g / (1.0 + jnp.exp(-g)) * (ffn_scale * t[rows:])
        hid_send[:, off : off + wide] = hid.astype(BF16)
        window = pl.ds(off, wide)
        copies = [
            send(hid_send.at[:, window], hid_all.at[kv, :, window],
                 hid_s.at[i, d], hid_r.at[i, d], {"kv": p})
            for d, p in enumerate(kv_peer)
        ]
        hid_copies.append(copies)
        pending += copies
    hid_all[kv] = hid_send[...]
    late[4].wait()
    down = None
    for i, (off, width, wide) in enumerate(chunks):
        for c in hid_copies[i]:
            c.wait_recv()
        h = jnp.concatenate(
            [hid_all[k, :, off : off + width].astype(F32) for k in range(nkv)], axis=0
        ).astype(BF16)
        part = jnp.dot(h, wd[off : off + width, :], preferred_element_type=F32)
        down = part if down is None else down + part
    for j in range(ntp):
        dn_send[j] = down[:, j * tcols : (j + 1) * tcols].astype(BF16)
    copies = [
        send(dn_send.at[p], dn_recv.at[tp], dn_s.at[d], dn_r.at[d], {"tp": p})
        for d, p in enumerate(tp_peer)
    ]
    pending += copies
    tot = dn_send[tp].astype(F32)
    for d, c in enumerate(copies):
        c.wait_recv()
        tot = tot + dn_recv[tp_src[d]].astype(F32)
    out_tokens[...] = (mid_own[...].astype(F32) + tot).astype(BF16)
    for c in pending:
        c.wait_send()
    c_out.wait()


def hand_over(tok, c, n, m, tok_out, c_out, n_out, m_out, tok_v, c_v, n_v, m_v, isem, osem):
    size = c.shape[0] // PARTS
    moves = []
    for i in range(PARTS):
        window = pl.ds(i * size, size)
        moves.append((c.at[window], c_v.at[window], c_out.at[window]))
    moves += [(tok, tok_v, tok_out), (n, n_v, n_out), (m, m_v, m_out)]
    into = [pltpu.make_async_copy(a, b, isem.at[i]) for i, (a, b, _) in enumerate(moves)]
    out = [pltpu.make_async_copy(b, o, osem.at[i]) for i, (_, b, o) in enumerate(moves)]
    for x in into:
        x.start()
    for x, y in zip(into, out):
        x.wait()
        y.start()
    for y in out:
        y.wait()


def layer(
    nkv, ntp, d_model,
    tokens, norm_gain, w_query, w_key, w_value, w_ogate, w_igate, w_fgate,
    igate_bias, fgate_bias, state_c, state_n, state_m, head_gain,
    w_out, ffn_gain, w_gate, w_up, w_down,
):
    seqs, tcols = tokens.shape
    rows = seqs // nkv
    depth, qk = w_query.shape
    vv = w_value.shape[1]
    half = qk + vv
    ff = w_gate.shape[1]
    nch = len(cuts(ff))
    wide = -(-ff // LANES) * LANES
    hbm = pl.BlockSpec(memory_space=pl.ANY)
    vmem = pl.BlockSpec(memory_space=pltpu.VMEM)
    dma = lambda *n: pltpu.SemaphoreType.DMA(n)
    k, t = nkv - 1, ntp - 1
    smalls = (
        tokens, norm_gain.reshape(-1, LANES), w_igate.T, w_fgate.T, igate_bias[None],
        fgate_bias[None], state_n, state_m.T, head_gain, ffn_gain.reshape(-1, LANES),
    )
    scratch = [pltpu.VMEM(x.shape, x.dtype) for x in smalls] + [
        pltpu.VMEM((depth, 2 * half), BF16),
        pltpu.VMEM(w_out.shape, BF16),
        pltpu.VMEM(w_gate.shape[::-1], BF16),
        pltpu.VMEM(w_up.shape[::-1], BF16),
        pltpu.VMEM(w_down.shape, BF16),
        pltpu.VMEM(state_c.shape, F32),
        pltpu.VMEM(state_c.shape, F32),
        pltpu.VMEM((ntp, seqs, tcols), BF16),
        pltpu.VMEM((seqs, depth), BF16),
        pltpu.VMEM((nkv, 2 * rows, half), BF16),
        pltpu.VMEM((nkv, 2 * rows, half), BF16),
        pltpu.VMEM((nkv, rows, LANES), F32),
        pltpu.VMEM((nkv, rows, LANES), F32),
        pltpu.VMEM((rows, vv), F32),
        pltpu.VMEM((rows, vv), BF16),
        pltpu.VMEM((nkv, rows, vv), BF16),
        pltpu.VMEM((ntp, seqs, tcols), BF16),
        pltpu.VMEM((ntp, seqs, tcols), BF16),
        pltpu.VMEM((seqs, tcols), BF16),
        pltpu.VMEM((ntp, seqs, tcols), BF16),
        pltpu.VMEM((nkv, rows, LANES), F32),
        pltpu.VMEM((nkv, rows, LANES), F32),
        pltpu.VMEM((nkv, 2 * rows, wide), BF16),
        pltpu.VMEM((nkv, 2 * rows, wide), BF16),
        pltpu.VMEM((rows, wide), BF16),
        pltpu.VMEM((nkv, rows, wide), BF16),
        pltpu.VMEM((ntp, seqs, tcols), BF16),
        pltpu.VMEM((ntp, seqs, tcols), BF16),
        dma(9),
        pltpu.SemaphoreType.DMA,
        dma(len(smalls)),
        dma(t), dma(t), dma(k), dma(k), dma(k), dma(k), dma(k), dma(k), dma(t), dma(t), dma(t), dma(t),
        dma(k), dma(k), dma(nch, k), dma(nch, k), dma(nch, k), dma(nch, k), dma(t), dma(t),
    ]
    out = pl.pallas_call(
        functools.partial(kernel, nkv, ntp, d_model),
        out_shape=(
            jax.ShapeDtypeStruct(tokens.shape, BF16),
            jax.ShapeDtypeStruct(state_c.shape, F32),
            jax.ShapeDtypeStruct(state_n.shape, F32),
            jax.ShapeDtypeStruct(state_m.shape[::-1], F32),
        ),
        in_specs=[hbm] * 19,
        out_specs=(vmem, hbm, vmem, vmem),
        scratch_shapes=scratch,
        compiler_params=pltpu.CompilerParams(
            collective_id=0, has_side_effects=True, vmem_limit_bytes=60 * 1024 * 1024
        ),
    )(
        *smalls[:2], w_query, w_key, w_value, w_ogate, *smalls[2:6], state_c, *smalls[6:9],
        w_out, smalls[9], w_gate.T, w_up.T, w_down,
    )
    tok, new_c, new_n, new_m = pl.pallas_call(
        hand_over,
        out_shape=tuple(jax.ShapeDtypeStruct(o.shape, o.dtype) for o in out),
        in_specs=[hbm] * 4,
        out_specs=(hbm,) * 4,
        scratch_shapes=[pltpu.VMEM(o.shape, o.dtype) for o in out] + [dma(PARTS + 3), dma(PARTS + 3)],
    )(*out)
    return tok, new_c, new_n, new_m.T


def cell_update(query, key_vec, value_vec, igate, fgate, state_c, state_n, state_m):
    carried = jax.nn.log_sigmoid(fgate) + state_m
    new_m = jnp.maximum(carried, igate)
    keep_weight = jnp.exp(carried - new_m)
    write_weight = jnp.exp(igate - new_m)
    new_c = (
        keep_weight[..., None, None] * state_c
        + write_weight[..., None, None] * key_vec[..., :, None] * value_vec[..., None, :]
    )
    new_n = keep_weight[..., None] * state_n + write_weight[..., None] * key_vec
    numerator = jnp.einsum("bhd,bhde->bhe", query, new_c, precision=lax.Precision.HIGHEST)
    denominator = jnp.sum(query * new_n, axis=-1)
    head_out = numerator / jnp.maximum(jnp.abs(denominator), jnp.exp(-new_m))[..., None]
    return (new_c, new_n, new_m, head_out)


def plain_layer(
    tokens,
    norm_gain,
    w_query,
    w_key,
    w_value,
    w_ogate,
    w_igate,
    w_fgate,
    igate_bias,
    fgate_bias,
    state_c,
    state_n,
    state_m,
    head_gain,
    w_out,
    ffn_gain,
    w_gate,
    w_up,
    w_down,
):
    seq_rows = state_c.shape[0]
    heads_here, DK, DV = state_c.shape[1:]
    D = w_query.shape[0] * lax.axis_size("kv")
    token_cols = lax.all_gather(tokens, "tp", axis=1, tiled=True)
    token_vals = token_cols.astype(jnp.float32)
    normed = (token_vals * norm_gain.astype(jnp.float32)).astype(jnp.bfloat16)
    squares = jnp.sum(token_vals * token_vals, axis=1)
    part_query = jnp.dot(normed, w_query, preferred_element_type=jnp.float32)
    part_key = jnp.dot(normed, w_key, preferred_element_type=jnp.float32)
    part_value = jnp.dot(normed, w_value, preferred_element_type=jnp.float32)
    part_ogate = jnp.dot(normed, w_ogate, preferred_element_type=jnp.float32)
    part_igate = jnp.dot(normed, w_igate, preferred_element_type=jnp.float32)
    part_fgate = jnp.dot(normed, w_fgate, preferred_element_type=jnp.float32)
    all_squares = lax.psum(squares, "kv")
    sum_squares = lax.dynamic_slice_in_dim(
        all_squares, lax.axis_index("kv") * seq_rows, seq_rows, 0
    )
    sum_query, sum_key, sum_value, sum_ogate, sum_igate, sum_fgate = (
        lax.psum_scatter(part_query, "kv", scatter_dimension=0, tiled=True),
        lax.psum_scatter(part_key, "kv", scatter_dimension=0, tiled=True),
        lax.psum_scatter(part_value, "kv", scatter_dimension=0, tiled=True),
        lax.psum_scatter(part_ogate, "kv", scatter_dimension=0, tiled=True),
        lax.psum_scatter(part_igate, "kv", scatter_dimension=0, tiled=True),
        lax.psum_scatter(part_fgate, "kv", scatter_dimension=0, tiled=True),
    )
    row_scale = lax.rsqrt(sum_squares / D + NORM_EPS)[:, None]
    query = (row_scale * sum_query).reshape(seq_rows, heads_here, DK)
    key_vec = (row_scale * sum_key).reshape(seq_rows, heads_here, DK) * DK ** (-0.5)
    value_vec = (row_scale * sum_value).reshape(seq_rows, heads_here, DV)
    ogate = (row_scale * sum_ogate).reshape(seq_rows, heads_here, DV)
    igate = IGATE_CAP * jnp.tanh((row_scale * sum_igate + igate_bias) / IGATE_CAP)
    fgate = row_scale * sum_fgate + fgate_bias
    new_c, new_n, new_m, head_out = cell_update(
        query, key_vec, value_vec, igate, fgate, state_c, state_n, state_m
    )
    merged = (
        (head_out * head_gain.astype(jnp.float32) * jax.nn.sigmoid(ogate))
        .reshape(seq_rows, heads_here * DV)
        .astype(jnp.bfloat16)
    )
    attn_part = jnp.dot(
        lax.all_gather(merged, "kv", axis=0, tiled=True), w_out, preferred_element_type=jnp.float32
    )
    attn_out = lax.psum_scatter(
        attn_part.astype(jnp.bfloat16), "tp", scatter_dimension=1, tiled=True
    ).astype(jnp.float32)
    middle = (tokens.astype(jnp.float32) + attn_out).astype(jnp.bfloat16)
    middle_cols = lax.all_gather(middle, "tp", axis=1, tiled=True)
    middle_vals = middle_cols.astype(jnp.float32)
    normed_two = (middle_vals * ffn_gain.astype(jnp.float32)).astype(jnp.bfloat16)
    squares_two = jnp.sum(middle_vals * middle_vals, axis=1)
    gate_part = jnp.dot(normed_two, w_gate, preferred_element_type=jnp.float32)
    up_part = jnp.dot(normed_two, w_up, preferred_element_type=jnp.float32)
    gate_sum, up_sum, total_two = (
        lax.psum(gate_part.astype(jnp.bfloat16), "kv").astype(jnp.float32),
        lax.psum(up_part.astype(jnp.bfloat16), "kv").astype(jnp.float32),
        lax.psum(squares_two.astype(jnp.bfloat16), "kv").astype(jnp.float32),
    )
    ffn_scale = lax.rsqrt(total_two / D + NORM_EPS)[:, None]
    hidden = (jax.nn.silu(ffn_scale * gate_sum) * (ffn_scale * up_sum)).astype(jnp.bfloat16)
    down_part = jnp.dot(hidden, w_down, preferred_element_type=jnp.float32)
    down_out = lax.psum_scatter(
        down_part.astype(jnp.bfloat16), "tp", scatter_dimension=1, tiled=True
    ).astype(jnp.float32)
    out_tokens = (middle.astype(jnp.float32) + down_out).astype(jnp.bfloat16)
    return (out_tokens, new_c, new_n, new_m)


def solution(mesh):
    nkv, ntp = mesh.shape["kv"], mesh.shape["tp"]
    placed = (
        P("grp", ("kv", "tp")),
        P("kv"),
        P("kv", "tp"),
        P("kv", "tp"),
        P("kv", "tp"),
        P("kv", "tp"),
        P("kv", "tp"),
        P("kv", "tp"),
        P("tp"),
        P("tp"),
        P(("grp", "kv"), "tp", None, None),
        P(("grp", "kv"), "tp", None),
        P(("grp", "kv"), "tp"),
        P("tp", None),
        P("tp", "kv"),
        P("kv"),
        P("kv", "tp"),
        P("kv", "tp"),
        P("tp", "kv"),
    )

    def body(*args):
        d_model = args[2].shape[0] * nkv
        seqs, tcols = args[0].shape
        qk, vv = args[2].shape[1], args[4].shape[1]
        whole_tiles = tcols % LANES == 0 and qk % LANES == 0 and vv % LANES == 0
        if not whole_tiles or (seqs // nkv) % 8:
            return plain_layer(*args)
        return layer(nkv, ntp, d_model, *args)

    return jax.shard_map(
        body,
        mesh=mesh,
        in_specs=placed,
        out_specs=(
            P("grp", ("kv", "tp")),
            P(("grp", "kv"), "tp", None, None),
            P(("grp", "kv"), "tp", None),
            P(("grp", "kv"), "tp"),
        ),
        check_vma=False,
    )
```
